32 devices in a mesh: dp: 4 (over y, x), kv: 4 (over z), tp: 2 (over core).
Axes of the slice: x: 2, y: 2, z: 4, core: 2. Of those that a mesh axis runs over, the one named last changes fastest.
Arguments:
- tokens: bfloat16 [2048, 2048], P('dp', 'kv'), may hold values from -70 to 70
- pre_gain: float32 [2048], replicated, may hold values from 0.1 to 1.9
- query_weight: bfloat16 [2048, 1024], P(None, 'tp'), may hold values from -0.125 to 0.125
- key_weight: bfloat16 [2048, 1024], P(None, 'tp'), may hold values from -0.125 to 0.125
- value_weight: bfloat16 [2048, 1024], P(None, 'tp'), may hold values from -0.125 to 0.125
- gate_weight: bfloat16 [2048, 1024], P(None, 'tp'), may hold values from -0.125 to 0.125
- beta_weight: bfloat16 [2048, 8], replicated, may hold values from -0.125 to 0.125
- decay_weight: bfloat16 [2048, 8], replicated, may hold values from -0.125 to 0.125
- decay_log: float32 [8], P('tp'), may hold values from -3 to 0.5
- head_gain: float32 [128], replicated, may hold values from 0.1 to 1.9
- out_weight: bfloat16 [1024, 2048], P('tp', 'kv'), may hold values from -1 to 1
- post_gain: float32 [2048], P(('kv', 'tp')), may hold values from 0.1 to 1.9
- saved_state: float32 [512, 8, 128, 128], P(('dp', 'kv'), 'tp'), may hold values from -4 to 4
- earlier_keys: bfloat16 [512, 4, 8, 128], P(('dp', 'kv'), None, 'tp'), may hold values from -6 to 6
- earlier_values: bfloat16 [512, 4, 8, 128], P(('dp', 'kv'), None, 'tp'), may hold values from -6 to 6
- earlier_rates: float32 [512, 4, 8], P(('dp', 'kv'), None, 'tp'), may hold values from 0.05 to 0.95
- earlier_decays: float32 [512, 4, 8], P(('dp', 'kv'), None, 'tp'), may hold values from -1.5 to -0.02
- accepted: int32 [512], P(('dp', 'kv')), may hold values from 0 to 4
Outputs:
- mixed: bfloat16 [2048, 2048], P('dp', ('kv', 'tp'))
- committed: float32 [512, 8, 128, 128], P(('dp', 'kv'), 'tp')
The draws below stay inside these ranges and needn't reach their ends.
All inputs are finite; a program needn't handle non-finite values.
Results may differ from the reference program's by a relative error of at most 0.011.
Values may be sent and summed in bfloat16 or wider, within the bound.
A program may use at most 128 MiB of HBM per device.

```python
import jax
import jax.numpy as jnp
from jax import lax

D = 2048
HEADS = 8
HEAD = 128
PROPOSALS = 4
SEQS = 512
ROWS = 2048


def draw_tokens(key, part):
    columns = jnp.arange(D, dtype=jnp.float32)
    rising = 1.0 + 3.0 * columns / D
    base = jnp.clip(jax.random.normal(key, (ROWS, D), jnp.float32), -5.0, 5.0)
    return (base * rising).astype(jnp.bfloat16)


def draw_out_weight(key, part):
    columns = jnp.arange(D, dtype=jnp.float32)
    rising = (1.0 + 3.0 * columns / D) * (HEADS * HEAD) ** (-0.5)
    base = jnp.clip(jax.random.normal(key, (HEADS * HEAD, D), jnp.float32), -6.0, 6.0)
    return jnp.clip(base * rising, -1.0, 1.0).astype(jnp.bfloat16)


def place_ends(entries, stream_key, smallest, top_value):
    dims = entries.shape
    spot = [jax.random.randint(jax.random.fold_in(stream_key, axis), (), 0, dims[axis]) for axis in range(len(dims))]
    entries = entries.at[tuple(spot)].set(smallest)
    longest = dims.index(max(dims))
    spot[longest] = (spot[longest] + 1) % dims[longest]
    return entries.at[tuple(spot)].set(top_value)


def level_of(key, extent, cuts, least, high):
    def one(dim, shards_of):
        heights = jax.random.uniform(jax.random.fold_in(jax.random.fold_in(key, 6), dim), (shards_of,), jnp.float32, least / len(cuts), high / len(cuts))
        return jnp.repeat(jnp.exp(heights), extent[dim] // shards_of).reshape((-1,) + (1,) * (len(extent) - dim - 1))

    loudness = one(*cuts[0])
    for cut in cuts[1:]:
        loudness = loudness * one(*cut)
    return loudness


def normal_values(rng, extent, deviation, most, cuts=(), kind=jnp.bfloat16):
    values = deviation * jax.random.normal(rng, extent, jnp.float32)
    if cuts:
        values = values * level_of(rng, extent, cuts, -0.22, 0.18)
    return jnp.clip(values, -most, most).astype(kind)


def setup_inputs(seed: int = 0) -> dict:
    splits = jax.random.split(jax.random.key(seed), 19)
    return {
        "tokens": draw_tokens(jax.random.fold_in(splits[18], 71), 0),
        "pre_gain": jnp.clip(1.0 + 0.18 * jax.random.normal(splits[1], (D,), jnp.float32), 0.1, 1.9),
        "query_weight": normal_values(splits[2], (D, HEADS * HEAD), D ** -0.5, 0.125, ((1, 2),)),
        "key_weight": normal_values(splits[3], (D, HEADS * HEAD), D ** -0.5, 0.125, ((1, 2),)),
        "value_weight": normal_values(splits[4], (D, HEADS * HEAD), D ** -0.5, 0.125, ((1, 2),)),
        "gate_weight": normal_values(splits[5], (D, HEADS * HEAD), D ** -0.5, 0.125, ((1, 2),)),
        "beta_weight": normal_values(splits[6], (D, HEADS), D ** -0.5, 0.125),
        "decay_weight": normal_values(splits[7], (D, HEADS), D ** -0.5, 0.125),
        "decay_log": jnp.clip(-3.0 + 3.5 * jax.random.uniform(splits[8], (HEADS,), jnp.float32) ** level_of(splits[8], (HEADS,), ((0, 2),), -0.2, 0.2), -3.0, 0.5),
        "head_gain": jnp.clip(1.0 + 0.18 * jax.random.normal(splits[9], (HEAD,), jnp.float32), 0.1, 1.9),
        "out_weight": draw_out_weight(jax.random.fold_in(splits[18], 71), 0),
        "post_gain": jnp.clip(1.0 + 0.18 * jax.random.normal(splits[11], (D,), jnp.float32), 0.1, 1.9),
        "saved_state": normal_values(splits[12], (SEQS, HEADS, HEAD, HEAD), 0.3, 4.0, ((0, 16), (1, 2)), jnp.float32),
        "earlier_keys": normal_values(splits[13], (SEQS, PROPOSALS, HEADS, HEAD), 1.0, 6.0, ((0, 16), (2, 2))),
        "earlier_values": normal_values(splits[14], (SEQS, PROPOSALS, HEADS, HEAD), 1.0, 6.0, ((0, 16), (2, 2))),
        "earlier_rates": jnp.clip(0.05 + 0.9 * jax.random.uniform(splits[15], (SEQS, PROPOSALS, HEADS), jnp.float32) ** level_of(splits[15], (SEQS, PROPOSALS, HEADS), ((0, 16), (2, 2)), -0.2, 0.2), 0.05, 0.95),
        "earlier_decays": jnp.clip(-1.5 + 1.48 * jax.random.uniform(splits[16], (SEQS, PROPOSALS, HEADS), jnp.float32) ** level_of(splits[16], (SEQS, PROPOSALS, HEADS), ((0, 16), (2, 2)), -0.2, 0.2), -1.5, -0.02),
        "accepted": place_ends(jax.random.randint(splits[17], (SEQS,), 0, PROPOSALS + 1), jax.random.fold_in(splits[17], 1), 0, PROPOSALS).astype(jnp.int32),
    }


def unit_norm(values):
    return values * lax.rsqrt(lax.optimization_barrier(jnp.sum(values * values, axis=-1, keepdims=True)) + 1e-06)

def advance(current, key_row, value_row, rate_now, log_decay):
    recalled = lax.optimization_barrier(jnp.sum(key_row[..., :, None] * current, axis=-2))
    rate_cube = rate_now[..., None, None]
    current = current - rate_cube * key_row[..., :, None] * recalled[..., None, :]
    return jnp.exp(log_decay)[..., None, None] * current + rate_cube * key_row[..., :, None] * value_row[..., None, :]

def run_heads(saved_state, earlier_keys, earlier_values, earlier_rates, earlier_decays, accepted, queries, keys_unit, values_act, rates, decays):
    current = saved_state
    proposals = earlier_keys.shape[1]
    for position in range(proposals):
        live = (position < accepted).astype(jnp.float32)
        live = live.reshape(live.shape + (1,) * (earlier_rates.ndim - 2))
        current = advance(current, earlier_keys[:, position], earlier_values[:, position], earlier_rates[:, position] * live, earlier_decays[:, position] * live)
    committed = current
    outputs = []
    for position in range(proposals):
        current = advance(current, keys_unit[:, position], values_act[:, position], rates[:, position], decays[:, position])
        outputs.append(lax.optimization_barrier(jnp.sum(queries[:, position][..., :, None] * current, axis=-2)))
    return (committed, jnp.stack(outputs, axis=1))

def reference(tokens, pre_gain, query_weight, key_weight, value_weight, gate_weight, beta_weight, decay_weight, decay_log, head_gain, out_weight, post_gain, saved_state, earlier_keys, earlier_values, earlier_rates, earlier_decays, accepted):
    widened = tokens.astype(jnp.float32)
    inverse = lax.rsqrt(lax.optimization_barrier(jnp.mean(widened * widened, axis=1, keepdims=True)) + 1e-06)
    scaled = (widened * pre_gain).astype(jnp.bfloat16)

    def project(weight):
        return jnp.dot(scaled, weight, preferred_element_type=jnp.float32) * inverse

    def heads_of(values):
        return values.reshape(SEQS, PROPOSALS, HEADS, HEAD)
    queries = unit_norm(jax.nn.silu(heads_of(project(query_weight)))) * HEAD ** (-0.5)
    keys_unit = unit_norm(jax.nn.silu(heads_of(project(key_weight))))
    values_act = jax.nn.silu(heads_of(project(value_weight)))
    gates_raw = heads_of(project(gate_weight))
    rates = jax.nn.sigmoid(project(beta_weight)).reshape(SEQS, PROPOSALS, HEADS)
    decays = -jnp.exp(decay_log) * jax.nn.softplus(project(decay_weight)).reshape(SEQS, PROPOSALS, HEADS)
    earlier_unit = unit_norm(earlier_keys.astype(jnp.float32))
    earlier_vals = earlier_values.astype(jnp.float32)

    def per_head(items):
        return run_heads(items[0], items[1], items[2], items[3], items[4], accepted, items[5], items[6], items[7], items[8], items[9])
    items = (jnp.moveaxis(saved_state, 1, 0), jnp.moveaxis(earlier_unit, 2, 0), jnp.moveaxis(earlier_vals, 2, 0), jnp.moveaxis(earlier_rates, 2, 0), jnp.moveaxis(earlier_decays, 2, 0), jnp.moveaxis(queries, 2, 0), jnp.moveaxis(keys_unit, 2, 0), jnp.moveaxis(values_act, 2, 0), jnp.moveaxis(rates, 2, 0), jnp.moveaxis(decays, 2, 0))
    committed, reads = lax.map(per_head, items)
    committed = jnp.moveaxis(committed, 0, 1)
    reads = jnp.moveaxis(reads, 0, 2)
    normed = reads * lax.rsqrt(lax.optimization_barrier(jnp.mean(reads * reads, axis=-1, keepdims=True)) + 1e-06) * head_gain
    attended = (normed * jax.nn.silu(gates_raw)).reshape(ROWS, HEADS * HEAD).astype(jnp.bfloat16)
    projected = jnp.dot(attended, out_weight, preferred_element_type=jnp.float32)
    factor = lax.rsqrt(lax.optimization_barrier(jnp.mean(projected * projected, axis=1, keepdims=True)) + 1e-06)
    mixed = (projected * factor * post_gain).astype(jnp.bfloat16)
    return (mixed, committed)
```

```python
import functools

import jax
import jax.numpy as jnp
from jax import lax
from jax.experimental import pallas as pl
from jax.experimental.pallas import tpu as pltpu
from jax.sharding import PartitionSpec as P

F32 = jnp.float32
BF16 = jnp.bfloat16
EPS = 1e-06
MESH_IDS = pl.DeviceIdType.MESH
VMEM_BYTES = 60 * 1024 * 1024


def mm(a, b):
    return jnp.dot(a, b, preferred_element_type=F32)


def mm_nt(a, b):
    return lax.dot_general(a, b, (((1,), (1,)), ((), ())), preferred_element_type=F32)


def mm_tn(a, b):
    return lax.dot_general(a, b, (((0,), (0,)), ((), ())), preferred_element_type=F32)


def mm_exact(a, b):
    return jnp.dot(a, b, preferred_element_type=F32, precision=lax.Precision.HIGHEST)


def unit(values):
    return values * lax.rsqrt(jnp.sum(values * values, axis=-1, keepdims=True) + EPS)


def silu(values):
    return values / (1.0 + jnp.exp(-values))


def masks_of(rows, proposals):
    r = lax.broadcasted_iota(jnp.int32, (rows, rows), 0)
    c = lax.broadcasted_iota(jnp.int32, (rows, rows), 1)
    same = (r // proposals) == (c // proposals)
    return same, same & (c <= r), same & (c < r)


def per_sequence(operands, state_of, proposals, rows):
    size = operands[0].shape[1]
    group = 16
    seqs = group // proposals
    stack = group * len(operands)
    row = lax.broadcasted_iota(jnp.int32, (stack, size), 0)
    owner = (row % group) // proposals
    outs = [[] for _ in operands]
    for g in range(rows // group):
        x = jnp.concatenate([o[g * group:(g + 1) * group] for o in operands], axis=0)
        lhs = jnp.concatenate(
            [jnp.where(owner == s, x, 0.0).astype(BF16) for s in range(seqs)], axis=1
        )
        rhs = state_of(g * seqs, seqs).reshape(seqs * size, size).astype(BF16)
        y = mm(lhs, rhs)
        for i in range(len(operands)):
            outs[i].append(y[i * group:(i + 1) * group])
    return [jnp.concatenate(o, axis=0) for o in outs]


def solve(keys, values, recalled, rate, decay_pairs, gamma, strict):
    kb = keys.astype(BF16)
    low = (jnp.where(strict, decay_pairs * mm_nt(kb, kb), 0.0) * rate).astype(BF16)
    rhs = rate * (values - gamma * recalled)
    square = mm(low, low).astype(BF16)
    x = rhs + mm(square, rhs.astype(BF16))
    return x - mm(low, x.astype(BF16))


def commit_kernel(proposals, heads, keys_ref, values_ref, bg_ref, state_ref, out_ref, cum, cum_t, last):
    h = pl.program_id(0)
    rows, size = keys_ref.shape
    same, incl, strict = masks_of(rows, proposals)

    bg = bg_ref[...]
    total = mm_exact(jnp.where(incl, 1.0, 0.0), bg)
    cum[...] = total
    cum_t[...] = total.T
    last[...] = mm_exact(jnp.where(same, 1.0, 0.0), bg)
    lane = lax.broadcasted_iota(jnp.int32, (rows, rows), 1)

    def column(ref, j):
        return jnp.sum(jnp.where(lane == j, ref[...], 0.0), axis=1, keepdims=True)

    rate = column(bg_ref, h)
    g_col = column(cum, heads + h)
    g_last = column(last, heads + h)
    g_row = cum_t[pl.ds(heads + h, 1), :]
    pairs = jnp.exp(jnp.where(incl, g_col - g_row, -1e30))
    keys = unit(keys_ref[...].astype(F32))
    (recalled,) = per_sequence(
        [keys], lambda s, n: state_ref[s:s + n, 0], proposals, rows
    )
    w = solve(keys, values_ref[...].astype(F32), recalled, rate, pairs, jnp.exp(g_col), strict)
    scaled_keys = (keys * jnp.exp(g_last - g_col)).astype(BF16)
    whole = jnp.broadcast_to(jnp.exp(g_last), (rows, size))
    group = 16
    seqs = group // proposals
    owner = lax.broadcasted_iota(jnp.int32, (group, size), 0) // proposals
    for g in range(rows // group):
        wg = w[g * group:(g + 1) * group]
        spread = jnp.concatenate(
            [jnp.where(owner == s, wg, 0.0).astype(BF16) for s in range(seqs)], axis=1
        )
        add = mm_tn(scaled_keys[g * group:(g + 1) * group], spread)
        for s in range(seqs):
            seq = g * seqs + s
            keep = whole[seq * proposals:seq * proposals + 1]
            out_ref[seq, 0] = keep * state_ref[seq, 0] + add[:, s * size:(s + 1) * size]


def layer_kernel(
    kv, tp, proposals, heads, model_width,
    tokens, gains, qw, kw, vw, gw, bd, log_row, head_gain, ow, post, state,
    out,
    tok, wv, sv, owv, acc, sacc, att, attall, part, give, take, sums, sumall,
    w_sem, s_sem, ow_sem, own_sem, tok_send, tok_recv, att_send, att_recv, own_att,
    tp_send, tp_recv, sum_send, sum_recv,
):
    me = lax.axis_index("kv")
    core = lax.axis_index("tp")
    rows, chunk = tok.shape[1], tok.shape[2]
    size = head_gain.shape[1]
    cols = out.shape[1]
    weights = (qw, kw, vw, gw)

    def source(d):
        return lax.rem(me - d + kv, kv)

    def target(d):
        return lax.rem(me + d, kv)

    local = {}
    local["tok"] = pltpu.make_async_copy(tokens.at[pl.ds(me * rows, rows), :], tok.at[0], own_sem)
    local["tok"].start()
    for d in range(kv):
        for i in range(4):
            local["w", i, d] = pltpu.make_async_copy(
                weights[i].at[pl.ds(source(d) * chunk, chunk), :], wv.at[i, d], w_sem.at[i, d]
            )
            local["w", i, d].start()
    for h in range(heads):
        local["s", h] = pltpu.make_async_copy(state.at[:, h], sv.at[h], s_sem.at[h])
        local["s", h].start()
    for o in range(tp):
        half = lax.rem(core + o, tp)
        if len(ow.shape) == 3:
            src = ow.at[half]
        else:
            src = ow.at[:, pl.ds(pl.multiple_of(half * cols, 128), cols)]
        local["o", o] = pltpu.make_async_copy(src, owv.at[o], ow_sem.at[o])
        local["o", o].start()

    barrier = pltpu.get_barrier_semaphore()
    group = kv * tp
    flat = me * tp + core

    def peer(o):
        other = lax.rem(flat + o, group)
        return {"kv": other // tp, "tp": lax.rem(other, tp)}

    for o in range(1, group):
        pl.semaphore_signal(barrier, inc=1, device_id=peer(o), device_id_type=MESH_IDS)
    pl.semaphore_wait(barrier, group - 1)

    sent = {}
    for d in range(1, kv):
        sent[d] = pltpu.make_async_remote_copy(
            src_ref=tokens.at[pl.ds(target(d) * rows, rows), :],
            dst_ref=tok.at[d],
            send_sem=tok_send.at[d],
            recv_sem=tok_recv.at[d],
            device_id={"kv": target(d)},
            device_id_type=MESH_IDS,
        )
        sent[d].start()

    squares = jnp.zeros((rows, 1), F32)
    for d in range(kv):
        if d == 0:
            local["tok"].wait()
        else:
            sent[d].wait_recv()
        c = source(d)
        wide = tok[d].astype(F32)
        squares = squares + jnp.sum(wide * wide, axis=1, keepdims=True)
        scaled = (wide * gains[pl.ds(c, 1), :]).astype(BF16)
        small = mm_nt(scaled, bd[:, pl.ds(pl.multiple_of(c * chunk, 128), chunk)])
        if d == 0:
            sacc[...] = small
        else:
            sacc[...] += small
        for i in range(4):
            local["w", i, d].wait()
            y = mm(scaled, wv[i, d])
            if d == 0:
                acc[i] = y
            else:
                acc[i] += y
    for d in range(1, kv):
        sent[d].wait_send()
    inverse = lax.rsqrt(squares / model_width + EPS)

    same, incl, strict = masks_of(rows, proposals)
    raw = sacc[...] * inverse
    rates = 1.0 / (1.0 + jnp.exp(-raw))
    soft = jnp.maximum(raw, 0.0) + jnp.log1p(jnp.exp(-jnp.abs(raw)))
    decays = -jnp.exp(log_row[...]) * soft
    cum = mm_exact(jnp.where(incl, 1.0, 0.0), decays)
    cum_t = cum.T
    moves = {}
    for h in range(heads):
        block = slice(h * size, (h + 1) * size)
        query = unit(silu(acc[0, :, block] * inverse)) * size ** (-0.5)
        key = unit(silu(acc[1, :, block] * inverse))
        value = silu(acc[2, :, block] * inverse)
        gate = silu(acc[3, :, block] * inverse)
        g_col = cum[:, heads + h:heads + h + 1]
        g_row = cum_t[heads + h:heads + h + 1, :]
        pairs = jnp.exp(jnp.where(incl, g_col - g_row, -1e30))
        gamma = jnp.exp(g_col)
        local["s", h].wait()
        recalled, asked = per_sequence(
            [key, query], lambda s, n: sv[h, s:s + n], proposals, rows
        )
        w = solve(key, value, recalled, rates[:, h:h + 1], pairs, gamma, strict)
        mix = (pairs * mm_nt(query.astype(BF16), key.astype(BF16))).astype(BF16)
        reads = gamma * asked + mm(mix, w.astype(BF16))
        normed = reads * lax.rsqrt(jnp.mean(reads * reads, axis=-1, keepdims=True) + EPS)
        att[h] = (normed * head_gain[...] * gate).astype(BF16)
        for d in range(1, kv):
            moves[d, h] = pltpu.make_async_remote_copy(
                src_ref=att.at[h],
                dst_ref=attall.at[d, h],
                send_sem=att_send.at[d, h],
                recv_sem=att_recv.at[d, h],
                device_id={"kv": target(d)},
                device_id_type=MESH_IDS,
            )
            moves[d, h].start()

    for o in range(tp):
        local["o", o].wait()
    swaps = {}
    for d in range(kv):
        for h in range(heads):
            if d:
                moves[d, h].wait_recv()
        if d:
            rows_in = jnp.concatenate([attall[d, h] for h in range(heads)], axis=1)
        else:
            rows_in = jnp.concatenate([att[h] for h in range(heads)], axis=1)
        for o in range(1, tp):
            give[d, o] = mm(rows_in, owv[o]).astype(BF16)
            swaps[d, o] = pltpu.make_async_remote_copy(
                src_ref=give.at[d, o],
                dst_ref=take.at[d, o],
                send_sem=tp_send.at[d, o],
                recv_sem=tp_recv.at[d, o],
                device_id={"tp": lax.rem(core + o, tp)},
                device_id_type=MESH_IDS,
            )
            swaps[d, o].start()
        part[d] = mm(rows_in, owv[0])
    ones = jnp.ones((8, cols), F32)
    for d in range(kv):
        for o in range(1, tp):
            swaps[d, o].wait_recv()
            part[d] += take[d, o].astype(F32)
        mine = part[d]
        line = lax.dot_general(
            ones, mine * mine, (((1,), (1,)), ((), ())),
            preferred_element_type=F32, precision=lax.Precision.HIGHEST,
        )
        sums[pl.ds(source(d), 1), :] = line[0:1]
    tells = {}
    for o in range(1, group):
        tells[o] = pltpu.make_async_remote_copy(
            src_ref=sums,
            dst_ref=sumall.at[o],
            send_sem=sum_send.at[o],
            recv_sem=sum_recv.at[o],
            device_id=peer(o),
            device_id_type=MESH_IDS,
        )
        tells[o].start()
    for key in moves:
        moves[key].wait_send()
    for key in swaps:
        swaps[key].wait_send()
    totals = sums[...]
    for o in range(1, group):
        tells[o].wait_recv()
        totals = totals + sumall[o]
    sums_factor = lax.rsqrt(totals / model_width + EPS)
    for o in range(1, group):
        tells[o].wait_send()
    sums[...] = sums_factor
    for d in range(kv):
        c = source(d)
        factor = jnp.broadcast_to(sums[pl.ds(c, 1), :], (rows, rows)).T[:, 0:1]
        out[pl.ds(pl.multiple_of(c * rows, rows), rows), :] = (
            part[d] * factor * post[...]
        ).astype(BF16)


def make_local(mesh):
    kv = mesh.shape["kv"]
    tp = mesh.shape["tp"]

    def local(
        tokens, pre_gain, query_weight, key_weight, value_weight, gate_weight, beta_weight,
        decay_weight, decay_log, head_gain, out_weight, post_gain, saved_state, earlier_keys,
        earlier_values, earlier_rates, earlier_decays, accepted,
    ):
        seqs, heads, size = saved_state.shape[:3]
        proposals = earlier_keys.shape[1]
        rows = seqs * proposals
        width = heads * size
        model_width = pre_gain.shape[0]
        chunk = tokens.shape[1]
        cols = post_gain.shape[0]
        head_start = lax.axis_index("tp") * heads

        live = (jnp.arange(proposals)[None, :] < accepted[:, None]).astype(F32)[:, :, None]
        bg = jnp.concatenate([earlier_rates * live, earlier_decays * live], axis=2)
        bg = jnp.pad(bg.reshape(rows, 2 * heads), ((0, 0), (0, rows - 2 * heads)))
        state_spec = pl.BlockSpec((seqs, 1, size, size), lambda h: (0, h, 0, 0))
        row_spec = pl.BlockSpec((rows, size), lambda h: (0, h))
        committed = pl.pallas_call(
            functools.partial(commit_kernel, proposals, heads),
            grid=(heads,),
            out_shape=jax.ShapeDtypeStruct(saved_state.shape, F32),
            in_specs=[row_spec, row_spec, pl.BlockSpec((rows, rows), lambda h: (0, 0)), state_spec],
            out_specs=state_spec,
            scratch_shapes=[pltpu.VMEM((rows, rows), F32)] * 3,
            compiler_params=pltpu.CompilerParams(vmem_limit_bytes=VMEM_BYTES),
            cost_estimate=pl.CostEstimate(
                flops=2 * saved_state.size * 2 * proposals,
                bytes_accessed=saved_state.size * 8,
                transcendentals=0,
            ),
            name="commit",
        )(
            earlier_keys.reshape(rows, width),
            earlier_values.reshape(rows, width),
            bg,
            saved_state,
        )

        beta_rows = lax.dynamic_slice_in_dim(beta_weight.T, head_start, heads, 0)
        decay_rows = lax.dynamic_slice_in_dim(decay_weight.T, head_start, heads, 0)
        bd = jnp.pad(
            jnp.concatenate([beta_rows, decay_rows], axis=0), ((0, rows - 2 * heads), (0, 0))
        )
        log_row = jnp.pad(decay_log, (heads, rows - 2 * heads)).reshape(1, rows)
        if cols % 128:
            out_w = jnp.moveaxis(out_weight.reshape(width, tp, cols), 1, 0)
        else:
            out_w = out_weight
        any_spec = pl.BlockSpec(memory_space=pl.ANY)
        vmem_spec = pl.BlockSpec(memory_space=pltpu.VMEM)
        dma = pltpu.SemaphoreType.DMA
        mixed = pl.pallas_call(
            functools.partial(layer_kernel, kv, tp, proposals, heads, model_width),
            out_shape=jax.ShapeDtypeStruct((tokens.shape[0], cols), BF16),
            in_specs=[any_spec, vmem_spec] + [any_spec] * 4 + [vmem_spec] * 3
            + [any_spec, vmem_spec, any_spec],
            out_specs=vmem_spec,
            scratch_shapes=[
                pltpu.VMEM((kv, rows, chunk), BF16),
                pltpu.VMEM((4, kv, chunk, width), BF16),
                pltpu.VMEM((heads, seqs, size, size), F32),
                pltpu.VMEM((tp, width, cols), BF16),
                pltpu.VMEM((4, rows, width), F32),
                pltpu.VMEM((rows, rows), F32),
                pltpu.VMEM((heads, rows, size), BF16),
                pltpu.VMEM((kv, heads, rows, size), BF16),
                pltpu.VMEM((kv, rows, cols), F32),
                pltpu.VMEM((kv, tp, rows, cols), BF16),
                pltpu.VMEM((kv, tp, rows, cols), BF16),
                pltpu.VMEM((kv, rows), F32),
                pltpu.VMEM((kv * tp, kv, rows), F32),
                dma((4, kv)), dma((heads,)), dma((tp,)), dma, dma((kv,)), dma((kv,)),
                dma((kv, heads)), dma((kv, heads)), dma,
                dma((kv, tp)), dma((kv, tp)), dma((kv * tp,)), dma((kv * tp,)),
            ],
            compiler_params=pltpu.CompilerParams(
                collective_id=0, has_side_effects=True, vmem_limit_bytes=VMEM_BYTES
            ),
            name="layer",
        )(
            tokens, pre_gain.reshape(kv, chunk), query_weight, key_weight, value_weight,
            gate_weight, bd, log_row, head_gain.reshape(1, size), out_w,
            post_gain.reshape(1, cols), committed,
        )
        return (mixed, committed)

    return local


def solution(mesh):
    placed = (
        P("dp", "kv"),
        P(),
        P(None, "tp"),
        P(None, "tp"),
        P(None, "tp"),
        P(None, "tp"),
        P(),
        P(),
        P("tp"),
        P(),
        P("tp", "kv"),
        P(("kv", "tp")),
        P(("dp", "kv"), "tp", None, None),
        P(("dp", "kv"), None, "tp", None),
        P(("dp", "kv"), None, "tp", None),
        P(("dp", "kv"), None, "tp"),
        P(("dp", "kv"), None, "tp"),
        P(("dp", "kv")),
    )
    return jax.shard_map(
        make_local(mesh),
        mesh=mesh,
        in_specs=placed,
        out_specs=(P("dp", ("kv", "tp")), P(("dp", "kv"), "tp", None, None)),
        check_vma=False,
    )
```

```python
import functools

import jax
import jax.numpy as jnp
from jax import lax
from jax.experimental import pallas as pl
from jax.experimental.pallas import tpu as pltpu
from jax.sharding import PartitionSpec as P

F32 = jnp.float32
BF16 = jnp.bfloat16
EPS = 1e-06
MESH_IDS = pl.DeviceIdType.MESH
VMEM_BYTES = 60 * 1024 * 1024


def mm(a, b):
    return jnp.dot(a, b, preferred_element_type=F32)


def mm_nt(a, b):
    return lax.dot_general(a, b, (((1,), (1,)), ((), ())), preferred_element_type=F32)


def mm_tn(a, b):
    return lax.dot_general(a, b, (((0,), (0,)), ((), ())), preferred_element_type=F32)


def mm_exact(a, b):
    return jnp.dot(a, b, preferred_element_type=F32, precision=lax.Precision.HIGHEST)


def unit(values):
    return values * lax.rsqrt(jnp.sum(values * values, axis=-1, keepdims=True) + EPS)


def silu(values):
    return values / (1.0 + jnp.exp(-values))


def masks_of(rows, proposals):
    r = lax.broadcasted_iota(jnp.int32, (rows, rows), 0)
    c = lax.broadcasted_iota(jnp.int32, (rows, rows), 1)
    same = (r // proposals) == (c // proposals)
    return same, same & (c <= r), same & (c < r)


def per_sequence(operands, state_of, proposals, rows):
    size = operands[0].shape[1]
    group = 16
    seqs = group // proposals
    stack = group * len(operands)
    row = lax.broadcasted_iota(jnp.int32, (stack, size), 0)
    owner = (row % group) // proposals
    outs = [[] for _ in operands]
    for g in range(rows // group):
        x = jnp.concatenate([o[g * group:(g + 1) * group] for o in operands], axis=0)
        lhs = jnp.concatenate(
            [jnp.where(owner == s, x, 0.0).astype(BF16) for s in range(seqs)], axis=1
        )
        rhs = state_of(g * seqs, seqs).reshape(seqs * size, size).astype(BF16)
        y = mm(lhs, rhs)
        for i in range(len(operands)):
            outs[i].append(y[i * group:(i + 1) * group])
    return [jnp.concatenate(o, axis=0) for o in outs]


def solve(keys, values, recalled, rate, decay_pairs, gamma, strict):
    kb = keys.astype(BF16)
    low = (jnp.where(strict, decay_pairs * mm_nt(kb, kb), 0.0) * rate).astype(BF16)
    rhs = rate * (values - gamma * recalled)
    square = mm(low, low).astype(BF16)
    x = rhs + mm(square, rhs.astype(BF16))
    return x - mm(low, x.astype(BF16))


def commit_kernel(proposals, keys_ref, values_ref, rates_ref, decays_ref, accepted_ref, state_ref, out_ref):
    h = pl.program_id(0)
    rows, size = keys_ref.shape
    seqs = accepted_ref.shape[1]
    same, incl, strict = masks_of(rows, proposals)
    row = lax.broadcasted_iota(jnp.int32, (rows, seqs), 0)
    own = (row // proposals) == lax.broadcasted_iota(jnp.int32, (rows, seqs), 1)

    def line(ref, p):
        return jnp.where(accepted_ref[...] > p, ref[p, pl.ds(h, 1), :], 0.0)

    def column(lines):
        spread = jnp.zeros((rows, seqs), F32)
        for p in range(proposals):
            spread = jnp.where(own & (row % proposals == p), lines[p], spread)
        return jnp.sum(spread, axis=1, keepdims=True)

    rate = column([line(rates_ref, p) for p in range(proposals)])
    sums = [line(decays_ref, 0)]
    for p in range(1, proposals):
        sums.append(sums[-1] + line(decays_ref, p))
    g_col = column(sums)
    g_last = column([sums[-1]] * proposals)
    g_row = jnp.broadcast_to(g_col, (rows, rows)).T
    pairs = jnp.exp(jnp.where(incl, g_col - g_row, -1e30))
    keys = unit(keys_ref[...].astype(F32))
    (recalled,) = per_sequence(
        [keys], lambda s, n: state_ref[s:s + n, 0], proposals, rows
    )
    w = solve(keys, values_ref[...].astype(F32), recalled, rate, pairs, jnp.exp(g_col), strict)
    scaled_keys = (keys * jnp.exp(g_last - g_col)).astype(BF16)
    whole = jnp.broadcast_to(jnp.exp(g_last), (rows, size))
    group = 16
    seqs = group // proposals
    owner = lax.broadcasted_iota(jnp.int32, (group, size), 0) // proposals
    for g in range(rows // group):
        wg = w[g * group:(g + 1) * group]
        spread = jnp.concatenate(
            [jnp.where(owner == s, wg, 0.0).astype(BF16) for s in range(seqs)], axis=1
        )
        add = mm_tn(scaled_keys[g * group:(g + 1) * group], spread)
        for s in range(seqs):
            seq = g * seqs + s
            keep = whole[seq * proposals:seq * proposals + 1]
            out_ref[seq, 0] = keep * state_ref[seq, 0] + add[:, s * size:(s + 1) * size]


def layer_kernel(
    kv, tp, proposals, heads, model_width,
    tokens, gains, qw, kw, vw, gw, beta_t, decay_t, log_rate, head_gain, ow, post, state,
    out,
    tok, wv, sv, owv, acc, bacc, dacc, att, passed, part, give, take, sums, sumall,
    w_sem, s_sem, ow_sem, own_sem, tok_send, tok_recv, half_send, half_recv, att_send, att_recv,
    tp_send, tp_recv, sum_send, sum_recv,
):
    me = lax.axis_index("kv")
    core = lax.axis_index("tp")
    rows, chunk = tok.shape[1], tok.shape[2]
    size = head_gain.shape[1]
    cols = out.shape[1]
    weights = (qw, kw, vw, gw)

    def source(d):
        return lax.rem(me - d + kv, kv)

    def target(d):
        return lax.rem(me + d, kv)

    local = {}
    local["tok"] = pltpu.make_async_copy(tokens.at[pl.ds(me * rows, rows), :], tok.at[0], own_sem)
    local["tok"].start()
    for d in range(kv):
        for i in range(4):
            local["w", i, d] = pltpu.make_async_copy(
                weights[i].at[pl.ds(source(d) * chunk, chunk), :], wv.at[i, d], w_sem.at[i, d]
            )
            local["w", i, d].start()
    for h in range(heads):
        local["s", h] = pltpu.make_async_copy(state.at[:, h], sv.at[h], s_sem.at[h])
        local["s", h].start()
    for o in range(tp):
        half = lax.rem(core + o, tp)
        if len(ow.shape) == 3:
            src = ow.at[half]
        else:
            src = ow.at[:, pl.ds(pl.multiple_of(half * cols, 128), cols)]
        local["o", o] = pltpu.make_async_copy(src, owv.at[o], ow_sem.at[o])
        local["o", o].start()

    barrier = pltpu.get_barrier_semaphore()
    group = kv * tp
    flat = me * tp + core

    def peer(o):
        other = lax.rem(flat + o, group)
        return {"kv": other // tp, "tp": lax.rem(other, tp)}

    for o in range(1, group):
        pl.semaphore_signal(barrier, inc=1, device_id=peer(o), device_id_type=MESH_IDS)
    pl.semaphore_wait(barrier, group - 1)

    part_rows = rows // tp
    mine_rows = pl.ds(pl.multiple_of(core * part_rows, part_rows), part_rows)
    sent = {}
    halves = {}
    for d in range(1, kv):
        sent[d] = pltpu.make_async_remote_copy(
            src_ref=tokens.at[
                pl.ds(pl.multiple_of(target(d) * rows + core * part_rows, part_rows), part_rows), :
            ],
            dst_ref=tok.at[d, mine_rows],
            send_sem=tok_send.at[d],
            recv_sem=tok_recv.at[d],
            device_id={"kv": target(d)},
            device_id_type=MESH_IDS,
        )
        sent[d].start()

    def hand_over(d):
        sent[d].wait_recv()
        for o in range(1, tp):
            halves[d, o] = pltpu.make_async_remote_copy(
                src_ref=tok.at[d, mine_rows],
                dst_ref=tok.at[d, mine_rows],
                send_sem=half_send.at[d, o],
                recv_sem=half_recv.at[d, o],
                device_id={"tp": lax.rem(core + o, tp)},
                device_id_type=MESH_IDS,
            )
            halves[d, o].start()

    def project(d, squares):
        if d == 0:
            local["tok"].wait()
        else:
            for o in range(1, tp):
                halves[d, o].wait_recv()
        c = source(d)
        span = pl.ds(pl.multiple_of(c * chunk, 128), chunk)
        wide = tok[d].astype(F32)
        scaled = (wide * gains[:, span]).astype(BF16)
        small_b = mm_nt(scaled, beta_t[:, span])
        small_d = mm_nt(scaled, decay_t[:, span])
        if d == 0:
            bacc[...] = small_b
            dacc[...] = small_d
        else:
            bacc[...] += small_b
            dacc[...] += small_d
        for i in range(4):
            local["w", i, d].wait()
            y = mm(scaled, wv[i, d])
            if d == 0:
                acc[i] = y
            else:
                acc[i] += y
        return squares + jnp.sum(wide * wide, axis=1, keepdims=True)

    squares = project(0, jnp.zeros((rows, 1), F32))
    for d in range(1, kv):
        hand_over(d)
        if d > 1:
            squares = project(d - 1, squares)
    if kv > 1:
        squares = project(kv - 1, squares)
    inverse = lax.rsqrt(squares / model_width + EPS)

    same, incl, strict = masks_of(rows, proposals)
    head_lane = lax.broadcasted_iota(jnp.int32, bacc.shape, 1)

    def column(values, h):
        return jnp.sum(jnp.where(head_lane == core * heads + h, values, 0.0), axis=1, keepdims=True)

    rates = 1.0 / (1.0 + jnp.exp(-bacc[...] * inverse))
    raw = dacc[...] * inverse
    soft = jnp.maximum(raw, 0.0) + jnp.log1p(jnp.exp(-jnp.abs(raw)))
    lane = lax.broadcasted_iota(jnp.int32, (rows, rows), 1)
    decays = jnp.zeros((rows, rows), F32)
    for h in range(heads):
        decay = -jnp.exp(jnp.full((rows, 1), log_rate[h], F32)) * column(soft, h)
        decays = jnp.where(lane == h, decay, decays)
    cum = mm_exact(jnp.where(incl, 1.0, 0.0), decays)
    cum_t = cum.T

    def hop(way, s, h):
        step = 1 if way == 0 else kv - 1
        return pltpu.make_async_remote_copy(
            src_ref=att.at[h] if s == 0 else passed.at[way, s, h],
            dst_ref=passed.at[way, s + 1, h],
            send_sem=att_send.at[way, s, h],
            recv_sem=att_recv.at[way, s + 1, h],
            device_id={"kv": lax.rem(me + step, kv)},
            device_id_type=MESH_IDS,
        )

    def arrives(way, s):
        return me - s >= 0 if way == 0 else me + s < kv

    def leaves(way):
        return me + 1 < kv if way == 0 else me >= 1

    def advance(turn):
        for s in range(kv):
            h = turn - s
            if not 0 <= h < heads:
                continue
            for way in range(2):
                if s == 0:
                    @pl.when(leaves(way))
                    def _():
                        hop(way, 0, h).start()
                else:
                    @pl.when(arrives(way, s))
                    def _():
                        hop(way, s - 1, h).wait_recv()
                    if s < kv - 1:
                        @pl.when(arrives(way, s) & leaves(way))
                        def _():
                            hop(way, s, h).start()

    def settle():
        for s in range(kv - 1):
            for way in range(2):
                @pl.when(arrives(way, s) & leaves(way))
                def _():
                    for h in range(heads):
                        hop(way, s, h).wait_send()

    for first in range(heads):
        batch = range(first, first + 1)
        local["s", first].wait()
        query, key, pairs, gamma, w, asked, reads = {}, {}, {}, {}, {}, {}, {}
        recalled = {}
        for h in batch:
            block = slice(h * size, (h + 1) * size)
            query[h] = unit(silu(acc[0, :, block] * inverse)) * size ** (-0.5)
            key[h] = unit(silu(acc[1, :, block] * inverse))
            pairs[h] = jnp.exp(jnp.where(incl, cum[:, h:h + 1] - cum_t[h:h + 1, :], -1e30))
            gamma[h] = jnp.exp(cum[:, h:h + 1])
        for h in batch:
            recalled[h], asked[h] = per_sequence(
                [key[h], query[h]], lambda s, n, h=h: sv[h, s:s + n], proposals, rows
            )
        for h in batch:
            value = silu(acc[2, :, h * size:(h + 1) * size] * inverse)
            w[h] = solve(key[h], value, recalled[h], column(rates, h), pairs[h], gamma[h], strict)
        for h in batch:
            mix = (pairs[h] * mm_nt(query[h].astype(BF16), key[h].astype(BF16))).astype(BF16)
            reads[h] = gamma[h] * asked[h] + mm(mix, w[h].astype(BF16))
        for h in batch:
            gate = silu(acc[3, :, h * size:(h + 1) * size] * inverse)
            scale = lax.rsqrt(jnp.mean(reads[h] * reads[h], axis=-1, keepdims=True) + EPS)
            att[h] = (reads[h] * scale * head_gain[...] * gate).astype(BF16)
        for h in batch:
            advance(h)

    for o in range(tp):
        local["o", o].wait()

    def swap(c, o):
        return pltpu.make_async_remote_copy(
            src_ref=give.at[c, o],
            dst_ref=take.at[c, o],
            send_sem=tp_send.at[c, o],
            recv_sem=tp_recv.at[c, o],
            device_id={"tp": lax.rem(core + o, tp)},
            device_id_type=MESH_IDS,
        )

    def combine(c, pieces):
        rows_in = jnp.concatenate(pieces, axis=1)
        for o in range(1, tp):
            give[c, o] = mm(rows_in, owv[o]).astype(BF16)
            swap(c, o).start()
        part[c] = mm(rows_in, owv[0])

    def finish(c):
        own = part[c]
        for o in range(1, tp):
            swap(c, o).wait_recv()
            own = own + take[c, o].astype(F32)
        part[c] = own
        total = jnp.sum(own * own, axis=1, keepdims=True)
        sums[pl.ds(c, 1), :] = jnp.broadcast_to(total, (rows, rows)).T[0:1]

    def blocks(turn):
        if turn < heads:
            return [(True, me, None)]
        s = turn - heads + 1
        return [(arrives(way, s), me - s if way == 0 else me + s, way) for way in range(2)]

    combine(me, [att[h] for h in range(heads)])
    for turn in range(heads, heads + kv - 1):
        advance(turn)
        s = turn - heads + 1
        for here, c, way in blocks(turn):
            @pl.when(here)
            def _():
                combine(c, [passed[way, s, h] for h in range(heads)])
        if s == 1:
            finish(me)
        else:
            for here, c, way in blocks(turn - 1):
                @pl.when(here)
                def _():
                    finish(c)
    if kv > 1:
        for here, c, way in blocks(heads + kv - 2):
            @pl.when(here)
            def _():
                finish(c)
    else:
        finish(me)
    tells = {}
    for o in range(1, group):
        tells[o] = pltpu.make_async_remote_copy(
            src_ref=sums,
            dst_ref=sumall.at[o],
            send_sem=sum_send.at[o],
            recv_sem=sum_recv.at[o],
            device_id=peer(o),
            device_id_type=MESH_IDS,
        )
        tells[o].start()
    settle()
    for d in range(1, kv):
        sent[d].wait_send()
        for o in range(1, tp):
            halves[d, o].wait_send()
    for c in range(kv):
        for o in range(1, tp):
            swap(c, o).wait_send()
    totals = sums[...]
    for o in range(1, group):
        tells[o].wait_recv()
        totals = totals + sumall[o]
    sums_factor = lax.rsqrt(totals / model_width + EPS)
    for o in range(1, group):
        tells[o].wait_send()
    for c in range(kv):
        factor = jnp.broadcast_to(sums_factor[c:c + 1, :], (rows, rows)).T[:, 0:1]
        out[c * rows:(c + 1) * rows, :] = (part[c] * factor * post[...]).astype(BF16)


def make_local(mesh):
    kv = mesh.shape["kv"]
    tp = mesh.shape["tp"]

    def local(
        tokens, pre_gain, query_weight, key_weight, value_weight, gate_weight, beta_weight,
        decay_weight, decay_log, head_gain, out_weight, post_gain, saved_state, earlier_keys,
        earlier_values, earlier_rates, earlier_decays, accepted,
    ):
        seqs, heads, size = saved_state.shape[:3]
        proposals = earlier_keys.shape[1]
        rows = seqs * proposals
        width = heads * size
        model_width = pre_gain.shape[0]
        chunk = tokens.shape[1]
        cols = post_gain.shape[0]
        state_spec = pl.BlockSpec((seqs, 1, size, size), lambda h: (0, h, 0, 0))
        row_spec = pl.BlockSpec((rows, size), lambda h: (0, h))
        scalar_spec = pl.BlockSpec((proposals, heads, seqs), lambda h: (0, 0, 0))
        committed = pl.pallas_call(
            functools.partial(commit_kernel, proposals),
            grid=(heads,),
            out_shape=jax.ShapeDtypeStruct(saved_state.shape, F32),
            in_specs=[
                row_spec, row_spec, scalar_spec, scalar_spec,
                pl.BlockSpec((1, seqs), lambda h: (0, 0)), state_spec,
            ],
            out_specs=state_spec,
            compiler_params=pltpu.CompilerParams(vmem_limit_bytes=VMEM_BYTES),
            cost_estimate=pl.CostEstimate(
                flops=2 * saved_state.size * 2 * proposals,
                bytes_accessed=saved_state.size * 8,
                transcendentals=0,
            ),
            name="commit",
        )(
            earlier_keys.reshape(rows, width),
            earlier_values.reshape(rows, width),
            jnp.transpose(earlier_rates, (1, 2, 0)),
            jnp.transpose(earlier_decays, (1, 2, 0)),
            accepted.reshape(1, seqs),
            saved_state,
        )

        if cols % 128:
            out_w = jnp.moveaxis(out_weight.reshape(width, tp, cols), 1, 0)
        else:
            out_w = out_weight
        any_spec = pl.BlockSpec(memory_space=pl.ANY)
        vmem_spec = pl.BlockSpec(memory_space=pltpu.VMEM)
        dma = pltpu.SemaphoreType.DMA
        mixed = pl.pallas_call(
            functools.partial(layer_kernel, kv, tp, proposals, heads, model_width),
            out_shape=jax.ShapeDtypeStruct((tokens.shape[0], cols), BF16),
            in_specs=[any_spec, vmem_spec] + [any_spec] * 4 + [vmem_spec] * 2
            + [pl.BlockSpec(memory_space=pltpu.SMEM), vmem_spec, any_spec, vmem_spec, any_spec],
            out_specs=vmem_spec,
            scratch_shapes=[
                pltpu.VMEM((kv, rows, chunk), BF16),
                pltpu.VMEM((4, kv, chunk, width), BF16),
                pltpu.VMEM((heads, seqs, size, size), F32),
                pltpu.VMEM((tp, width, cols), BF16),
                pltpu.VMEM((4, rows, width), F32),
                pltpu.VMEM((rows, heads * tp), F32),
                pltpu.VMEM((rows, heads * tp), F32),
                pltpu.VMEM((heads, rows, size), BF16),
                pltpu.VMEM((2, kv, heads, rows, size), BF16),
                pltpu.VMEM((kv, rows, cols), F32),
                pltpu.VMEM((kv, tp, rows, cols), BF16),
                pltpu.VMEM((kv, tp, rows, cols), BF16),
                pltpu.VMEM((kv, rows), F32),
                pltpu.VMEM((kv * tp, kv, rows), F32),
                dma((4, kv)), dma((heads,)), dma((tp,)), dma, dma((kv,)), dma((kv,)),
                dma((kv, tp)), dma((kv, tp)), dma((2, kv, heads)), dma((2, kv, heads)),
                dma((kv, tp)), dma((kv, tp)), dma((kv * tp,)), dma((kv * tp,)),
            ],
            compiler_params=pltpu.CompilerParams(
                collective_id=0, has_side_effects=True, vmem_limit_bytes=VMEM_BYTES
            ),
            name="layer",
        )(
            tokens, pre_gain.reshape(1, model_width), query_weight, key_weight, value_weight,
            gate_weight, beta_weight.T, decay_weight.T, decay_log, head_gain.reshape(1, size), out_w,
            post_gain.reshape(1, cols), committed,
        )
        return (mixed, committed)

    return local


def solution(mesh):
    placed = (
        P("dp", "kv"),
        P(),
        P(None, "tp"),
        P(None, "tp"),
        P(None, "tp"),
        P(None, "tp"),
        P(),
        P(),
        P("tp"),
        P(),
        P("tp", "kv"),
        P(("kv", "tp")),
        P(("dp", "kv"), "tp", None, None),
        P(("dp", "kv"), None, "tp", None),
        P(("dp", "kv"), None, "tp", None),
        P(("dp", "kv"), None, "tp"),
        P(("dp", "kv"), None, "tp"),
        P(("dp", "kv")),
    )
    return jax.shard_map(
        make_local(mesh),
        mesh=mesh,
        in_specs=placed,
        out_specs=(P("dp", ("kv", "tp")), P(("dp", "kv"), "tp", None, None)),
        check_vma=False,
    )
```
